32 devices in a mesh: sp: 8 (over z, x), tp: 4 (over y, core).
Axes of the slice: x: 2, y: 2, z: 4, core: 2. Of those that a mesh axis runs over, the one named last changes fastest.
Arguments:
- queries: bfloat16 [1024, 2048], P('sp', 'tp'), may hold values from -15 to 15
- key_rows: bfloat16 [1024, 2048], P('sp', 'tp'), may hold values from -6 to 6
- value_rows: bfloat16 [1024, 2048], P('sp', 'tp'), may hold values from -6 to 6
- break_bias: bfloat16 [1024, 16], P('sp', 'tp'), may hold values from -14 to 1
- stream: bfloat16 [1024, 4096], P('sp', 'tp'), may hold values from -24 to 24
- out_proj: bfloat16 [2048, 4096], P(None, 'tp'), may hold values from -0.5 to 0.5
- norm_gain: float32 [4096], P('tp'), may hold values from 0.1 to 1.9
- expert_ids: int32 [1024, 2], P('sp'), may hold values from 0 to 15, all different within a row; in each aligned block of 128 rows (0 to 127, 128 to 255, ...) at most 32 rows name the same one
- route_weights: float32 [1024, 2], P('sp'), may hold values from 0.1 to 2.5
- gate_proj: bfloat16 [16, 4096, 384], P('sp', 'tp'), may hold values from -0.09375 to 0.09375
- up_proj: bfloat16 [16, 4096, 384], P('sp', 'tp'), may hold values from -0.09375 to 0.09375
- down_proj: bfloat16 [16, 384, 4096], P('sp', None, 'tp'), may hold values from -0.3125 to 0.3125
- shared_gate: bfloat16 [4096, 384], P('tp'), may hold values from -0.09375 to 0.09375
- shared_up: bfloat16 [4096, 384], P('tp'), may hold values from -0.09375 to 0.09375
- shared_down: bfloat16 [384, 4096], P(None, 'tp'), may hold values from -0.3125 to 0.3125
Outputs:
- result: bfloat16 [1024, 4096], P('sp', 'tp')
The draws below stay inside these ranges and needn't reach their ends.
Inputs may be any that keep to these rules, and one draw needn't show every extreme that they name: `expert_ids`: each row names 2 different experts; within the rows of one index of sp no expert is named by more than 32 rows, a bound that some block reaches of them.
All inputs are finite; a program needn't handle non-finite values.
Results may differ from the reference program's by a relative error of at most 0.022.
Values may be sent and summed in bfloat16 or wider, within the bound.
A program may use at most 64 MiB of HBM per device.

```python
import math
import jax
import jax.numpy as jnp
import numpy as np
from jax import lax

D = 4096
ATTENTION_HEADS = 16
HD = 128
FFE = 384
FFS = 384
TOPK = 2
TOK_DEV = 128
SEQUENCE_TOKENS = 1024
EXPERTS = 16
CAP = 32
N_SP = 8
N_TP = 4


score_shift = 3.125


def draw_break_bias(key, part):
    every_key_rows = jax.random.split(jax.random.fold_in(key, 11), 5)
    fast_share = 0.5
    head_draw = jax.random.uniform(every_key_rows[0], (ATTENTION_HEADS,))
    fast_heads = head_draw < fast_share
    head_level = jnp.where(fast_heads, jnp.log(1.0 / 40.0), jnp.log(1.0 / SEQUENCE_TOKENS)) - score_shift
    block_shift = jax.random.uniform(every_key_rows[1], (SEQUENCE_TOKENS // TOK_DEV, ATTENTION_HEADS), minval=-0.7, maxval=0.7)
    jitter = 0.5 * jax.random.normal(every_key_rows[2], (SEQUENCE_TOKENS, ATTENTION_HEADS))
    logarithm_break_ratio = head_level[None, :] + jnp.repeat(block_shift, TOK_DEV, axis=0) + jitter
    stick_break_mask = jax.random.uniform(every_key_rows[3], (SEQUENCE_TOKENS, ATTENTION_HEADS)) < 4.0 / SEQUENCE_TOKENS
    break_probability = jax.random.uniform(every_key_rows[4], (SEQUENCE_TOKENS, ATTENTION_HEADS), minval=0.2, maxval=0.5)
    stick_break_level = jnp.log(break_probability / (1.0 - break_probability))
    return jnp.clip(jnp.where(stick_break_mask, stick_break_level, logarithm_break_ratio), -14.0, 1.0).astype(jnp.bfloat16)


def draw_stream(key, part):
    every_key_rows = jax.random.split(jax.random.fold_in(key, 23), 3)
    column_level = jnp.linspace(jnp.log(0.3), jnp.log(3.0), D) + 0.4 * jax.random.normal(every_key_rows[0], (D,))
    row_level = jax.random.uniform(every_key_rows[1], (SEQUENCE_TOKENS, 1), minval=jnp.log(0.15), maxval=jnp.log(1.5))
    base_values = jax.random.normal(every_key_rows[2], (SEQUENCE_TOKENS, D))
    scaled = base_values * jnp.exp(column_level)[None, :] * jnp.exp(row_level)
    return jnp.clip(scaled, -24.0, 24.0).astype(jnp.bfloat16)


def levels(rng, dims, shards, low, high):
    loudness, own = 1.0, jax.random.fold_in(rng, 6)
    for axis_at, blocks in shards:
        steps = jnp.exp(jax.random.uniform(jax.random.fold_in(own, axis_at), (blocks,), jnp.float32, low / len(shards), high / len(shards)))
        loudness = loudness * jnp.repeat(steps, dims[axis_at] // blocks).reshape([-1 if axis == axis_at else 1 for axis in range(len(dims))])
    return loudness


def deal_out(key, own, number, rows, amount, top, reach, lean):
    order = jax.random.permutation(key, amount)
    heavy_load, usual = shares(amount, rows * top, reach, lean, True), shares(amount, rows * top, reach, lean, False)
    places = jnp.arange(amount)

    def named(tallies, turn):
        used = int((tallies > 0).sum())
        fixed = max(1, used // 4)
        shifted = fixed + (places - fixed + turn * (used - fixed)) % max(1, amount - fixed)
        return jnp.zeros((amount,), jnp.int32).at[order[jnp.where(places < fixed, places, shifted)]].set(jnp.asarray(tallies, jnp.int32))

    tallies = jnp.where(number % 4 == 0, named(heavy_load, number // 4), named(usual, number - number // 4 - 1))
    mixed = jax.random.permutation(jax.random.fold_in(own, 3), amount)
    donor, receiver = mixed[0:amount // 2 * 2:2], mixed[1:amount // 2 * 2:2]
    room = jnp.minimum(tallies[donor] - 1, reach - tallies[receiver]) // 2
    room = jnp.where((donor == order[0]) | (receiver == order[0]) | (tallies[receiver] == 0), 0, jnp.maximum(room, 0))
    shifted = jax.random.randint(jax.random.fold_in(own, 4), (amount // 2,), 0, 1 << 20) % (room + 1)
    tallies = tallies.at[donor].add(-shifted).at[receiver].add(shifted)
    members = jnp.searchsorted(jnp.cumsum(tallies), jnp.arange(rows * top), side="right").astype(jnp.int32)
    table = members.reshape(top, rows).T
    table = table[jax.random.permutation(jax.random.fold_in(own, 1), rows)]
    turn = jax.random.randint(jax.random.fold_in(own, 2), (rows, 1), 0, top)
    return jnp.take_along_axis(table, (jnp.arange(top)[None, :] + turn) % top, axis=1)


def shares(number_of, total, bound, slope, full):
    portions = [(1 << 20) // math.isqrt(grade ** slope) + 1 for grade in range(1, number_of + 1)]
    largest = bound if full else min(bound, max(-(-total // number_of), total * portions[0] // sum(portions)))
    least = 1 if total - largest >= number_of - 1 else 0
    given, spare = [largest] + [least] * (number_of - 1), total - largest - least * (number_of - 1)
    while spare > 0:
        candidates = [i for i in range(1, number_of) if given[i] < largest] or [i for i in range(1, number_of) if given[i] < bound]
        pool, remaining = sum([portions[i] for i in candidates]), spare
        for i in candidates:
            more = min(bound - given[i], max(1, remaining * portions[i] // pool), spare)
            given[i] = given[i] + more
            spare = spare - more
    return np.array(given)


def normal_values(key, extent, deviation, bound, shards=(), held_as=jnp.bfloat16):
    loudness = levels(key, extent, shards, -0.22, 0.18) if shards else 1.0
    drawn = jax.random.normal(key, extent, jnp.float32) * deviation * loudness
    return jnp.minimum(jnp.maximum(drawn, -bound), bound).astype(held_as)


def setup_inputs(seed: int = 0) -> dict:
    streams_of = jax.random.split(jax.random.key(seed), 16)
    queries = normal_values(streams_of[0], (SEQUENCE_TOKENS, ATTENTION_HEADS * HD), 2.5, 15.0, ((0, 8), (1, 4)))
    key_rows = normal_values(streams_of[1], (SEQUENCE_TOKENS, ATTENTION_HEADS * HD), 1.0, 6.0, ((0, 8), (1, 4)))
    value_rows = normal_values(streams_of[2], (SEQUENCE_TOKENS, ATTENTION_HEADS * HD), 1.0, 6.0, ((0, 8), (1, 4)))
    break_bias = draw_break_bias(jax.random.fold_in(streams_of[15], 71), 0)
    stream = draw_stream(jax.random.fold_in(streams_of[15], 71), 0)
    out_proj = normal_values(streams_of[5], (ATTENTION_HEADS * HD, D), (ATTENTION_HEADS * HD // 16) ** -0.5, 0.5, ((1, 4),))
    norm_gain = jnp.clip(1.0 + 0.18 * jax.random.normal(streams_of[6], (D,), jnp.float32), 0.1, 1.9)
    expert_ids_keys = jax.random.split(jax.random.fold_in(streams_of[7], 1), SEQUENCE_TOKENS // TOK_DEV)
    expert_ids_turns = jax.random.permutation(jax.random.fold_in(streams_of[7], 3), SEQUENCE_TOKENS // TOK_DEV)
    expert_ids = jax.vmap(lambda own, number: deal_out(jax.random.fold_in(streams_of[7], 2), own, number, TOK_DEV, EXPERTS, TOPK, CAP, 2))(expert_ids_keys, expert_ids_turns).reshape((SEQUENCE_TOKENS, TOPK))
    route_weights = jnp.clip(jnp.exp(math.log(2.5) - 3.218876 * jax.random.uniform(streams_of[8], (SEQUENCE_TOKENS, TOPK), jnp.float32) ** levels(streams_of[8], (SEQUENCE_TOKENS, TOPK), ((0, 8),), -0.2, 0.2)), 0.1, 2.5)
    gate_proj = normal_values(streams_of[9], (EXPERTS, D, FFE), D ** -0.5, 0.09375, ((0, 8), (1, 4)))
    up_proj = normal_values(streams_of[10], (EXPERTS, D, FFE), D ** -0.5, 0.09375, ((0, 8), (1, 4)))
    down_proj = normal_values(streams_of[11], (EXPERTS, FFE, D), FFE ** -0.5, 0.3125, ((0, 8), (2, 4)))
    shared_gate = normal_values(streams_of[12], (D, FFS), D ** -0.5, 0.09375, ((0, 4),))
    shared_up = normal_values(streams_of[13], (D, FFS), D ** -0.5, 0.09375, ((0, 4),))
    shared_down = normal_values(streams_of[14], (FFS, D), FFS ** -0.5, 0.3125, ((1, 4),))
    return {"queries": queries, "key_rows": key_rows, "value_rows": value_rows, "break_bias": break_bias, "stream": stream, "out_proj": out_proj, "norm_gain": norm_gain, "expert_ids": expert_ids, "route_weights": route_weights, "gate_proj": gate_proj, "up_proj": up_proj, "down_proj": down_proj, "shared_gate": shared_gate, "shared_up": shared_up, "shared_down": shared_down}


EPS = 1e-06
query_block = 128

def stick_attention(queries, key_rows, value_rows, break_bias):
    head_q = queries.astype(jnp.float32).reshape(SEQUENCE_TOKENS, ATTENTION_HEADS, HD)
    head_k = key_rows.astype(jnp.float32).reshape(SEQUENCE_TOKENS, ATTENTION_HEADS, HD)
    head_v = value_rows.astype(jnp.float32).reshape(SEQUENCE_TOKENS, ATTENTION_HEADS, HD)
    bias_heads = break_bias.astype(jnp.float32).T
    key_pos = jnp.arange(SEQUENCE_TOKENS, dtype=jnp.int32)

    def one_block(block_index):
        offset = block_index * query_block
        query_part = lax.dynamic_slice_in_dim(head_q, offset, query_block, 0)
        positions = offset + jnp.arange(query_block, dtype=jnp.int32)
        logits = jnp.einsum('thd,shd->hts', query_part, head_k) * HD ** (-0.5) + bias_heads[:, None, :]
        before = (key_pos[None, :] < positions[:, None])[None]
        log_fail = jnp.where(before, jax.nn.log_sigmoid(-logits), 0.0)
        tail_sum = lax.cumsum(log_fail, axis=2, reverse=True) - log_fail
        weights = jnp.where(before, jnp.exp(jax.nn.log_sigmoid(logits) + tail_sum), 0.0)
        return jnp.einsum('hts,shd->thd', weights, head_v)
    outputs = lax.map(one_block, jnp.arange(SEQUENCE_TOKENS // query_block, dtype=jnp.int32))
    return outputs.reshape(SEQUENCE_TOKENS, ATTENTION_HEADS * HD).astype(jnp.bfloat16)

def block_sum(row_block, weight):
    feature_cut = row_block.shape[1] // N_TP

    def add_block(running, block_index):
        part_rows = lax.dynamic_slice_in_dim(row_block, block_index * feature_cut, feature_cut, 1)
        part_weight = lax.dynamic_slice_in_dim(weight, block_index * feature_cut, feature_cut, 0)
        partial_value = jnp.dot(part_rows, part_weight, preferred_element_type=jnp.float32).astype(jnp.bfloat16)
        partial_value = lax.optimization_barrier(partial_value)
        return (running + partial_value.astype(jnp.float32), None)
    start_sum = jnp.zeros((row_block.shape[0], weight.shape[1]), jnp.float32)
    running, _ = lax.scan(add_block, start_sum, jnp.arange(N_TP, dtype=jnp.int32))
    return running

def reference(queries, key_rows, value_rows, break_bias, stream, out_proj, norm_gain, expert_ids, route_weights, gate_proj, up_proj, down_proj, shared_gate, shared_up, shared_down):
    attended = stick_attention(queries, key_rows, value_rows, break_bias)
    mixed = (stream.astype(jnp.float32) + jnp.dot(attended, out_proj, preferred_element_type=jnp.float32)).astype(jnp.bfloat16)
    mixed = lax.optimization_barrier(mixed)
    mixed_f = mixed.astype(jnp.float32)
    inv_rms = lax.rsqrt(lax.optimization_barrier(jnp.mean(mixed_f * mixed_f, axis=1, keepdims=True)) + EPS)
    normed = (mixed_f * inv_rms * norm_gain[None, :]).astype(jnp.bfloat16)
    shared_hidden = (jax.nn.silu(block_sum(normed, shared_gate)) * block_sum(normed, shared_up)).astype(jnp.bfloat16)
    shared_out = jnp.dot(shared_hidden, shared_down, preferred_element_type=jnp.float32)
    rows_max = N_SP * CAP
    padded = jnp.concatenate([normed, jnp.zeros((1, D), jnp.bfloat16)], 0)

    def one_expert(running, expert):
        matches = expert_ids == expert
        chosen = jnp.any(matches, axis=1)
        weight_row = lax.optimization_barrier(jnp.sum(jnp.where(matches, route_weights, 0.0), axis=1))
        weight_pad = jnp.concatenate([weight_row, jnp.zeros((1,), jnp.float32)], 0)
        picked = jnp.nonzero(chosen, size=rows_max, fill_value=SEQUENCE_TOKENS)[0].astype(jnp.int32)
        row_block = padded[picked]
        gate_pre = block_sum(row_block, gate_proj[expert])
        up_pre = block_sum(row_block, up_proj[expert])
        hidden = (jax.nn.silu(gate_pre) * up_pre).astype(jnp.bfloat16)
        expert_out = jnp.dot(hidden, down_proj[expert], preferred_element_type=jnp.float32).astype(jnp.bfloat16)
        scaled = weight_pad[picked][:, None] * expert_out.astype(jnp.float32)
        return (running.at[picked].add(scaled), None)
    routed, _ = lax.scan(one_expert, jnp.zeros((SEQUENCE_TOKENS + 1, D), jnp.float32), jnp.arange(EXPERTS, dtype=jnp.int32))
    return (mixed_f + shared_out + routed[:SEQUENCE_TOKENS]).astype(jnp.bfloat16)
```

```python
import functools

import jax
import jax.numpy as jnp
from jax import lax
from jax.experimental import pallas as pl
from jax.experimental.pallas import tpu as pltpu
from jax.sharding import PartitionSpec as P

EPS = 1e-06
F32 = jnp.float32
BF16 = jnp.bfloat16


def attention_kernel(heads, hd, q_ref, kvb_ref, o_ref, acc, carry):
    tok = q_ref.shape[0]
    own = lax.axis_index("sp")
    scale = hd ** (-0.5)
    row = lax.broadcasted_iota(jnp.int32, (tok, tok), 0)
    col = lax.broadcasted_iota(jnp.int32, (tok, tok), 1)
    later = (row > col).astype(F32)
    sums = jnp.concatenate([later, jnp.ones((tok, tok), F32)], axis=1).astype(BF16)
    sums = jnp.concatenate([sums, sums], axis=0)
    pick_rows = max(16, heads)
    pick = (
        lax.broadcasted_iota(jnp.int32, (pick_rows, hd), 0)
        == lax.broadcasted_iota(jnp.int32, (pick_rows, hd), 1)
    ).astype(F32).astype(BF16)
    acc[...] = jnp.zeros_like(acc)
    carry[...] = jnp.zeros_like(carry)

    def block(j, diagonal):
        start = pl.multiple_of(j * tok, tok)
        piece = kvb_ref.at[pl.ds(start, tok)]
        bias = lax.dot_general(
            pick,
            piece[:, 2 * heads * hd : (2 * heads + 1) * hd],
            (((1,), (1,)), ((), ())),
            preferred_element_type=F32,
        )
        for h in range(heads):
            cols = slice(h * hd, (h + 1) * hd)
            z = lax.dot_general(
                q_ref[:, cols], piece[:, cols], (((1,), (1,)), ((), ())), preferred_element_type=F32
            )
            z = z * scale + bias[h : h + 1, :]
            low = jnp.log1p(jnp.exp(-jnp.abs(z)))
            fail = -(jnp.maximum(z, 0.0) + low)
            hit = jnp.minimum(z, 0.0) - low
            if diagonal:
                before = col < row
                fail = jnp.where(before, fail, 0.0)
            high = fail.astype(BF16)
            rest = (fail - high.astype(F32)).astype(BF16)
            both = jnp.dot(
                jnp.concatenate([high, rest], axis=1), sums, preferred_element_type=F32
            )
            before_sum = carry[h]
            w = jnp.exp(hit + both[:, :tok] + before_sum)
            if diagonal:
                w = jnp.where(before, w, 0.0)
            carry[h] = before_sum + both[:, tok:]
            acc[:, cols] += jnp.dot(
                w.astype(BF16),
                piece[:, heads * hd + h * hd : heads * hd + (h + 1) * hd],
                preferred_element_type=F32,
            )

    block(own, True)

    def step(i, _):
        block(own - 1 - i, False)
        return 0

    lax.fori_loop(0, own, step, 0)
    o_ref[...] = acc[...].astype(BF16)


def attention(queries, kvb, heads, hd):
    tok = queries.shape[0]
    vmem = pl.BlockSpec(memory_space=pltpu.VMEM)
    return pl.pallas_call(
        functools.partial(attention_kernel, heads, hd),
        out_shape=jax.ShapeDtypeStruct((tok, heads * hd), BF16),
        in_specs=[vmem, vmem],
        out_specs=vmem,
        scratch_shapes=[pltpu.VMEM((tok, heads * hd), F32), pltpu.VMEM((heads, tok, tok), F32)],
        compiler_params=pltpu.CompilerParams(vmem_limit_bytes=48 * 2**20),
        cost_estimate=pl.CostEstimate(flops=2 * 10**9, bytes_accessed=2**22, transcendentals=10**6),
    )(queries, kvb)


def body(
    queries,
    key_rows,
    value_rows,
    break_bias,
    stream,
    out_proj,
    norm_gain,
    expert_ids,
    route_weights,
    gate_proj,
    up_proj,
    down_proj,
    shared_gate,
    shared_up,
    shared_down,
):
    tok = queries.shape[0]
    heads = break_bias.shape[1]
    hd = queries.shape[1] // heads
    n_sp = lax.axis_size("sp")
    n_tp = lax.axis_size("tp")
    width = stream.shape[1] * n_tp
    hidden_width = gate_proj.shape[2]

    bias_wide = jnp.pad(break_bias, ((0, 0), (0, hd - heads)))
    kvb = jnp.concatenate([key_rows, value_rows, bias_wide], axis=1)
    kvb = lax.all_gather(kvb, "sp", axis=0, tiled=True)

    experts_local = gate_proj.shape[0]
    experts = experts_local * n_sp
    top_k = expert_ids.shape[1]
    cap = 2 * top_k * tok // experts
    expert_of = jnp.arange(experts, dtype=jnp.int32)
    named = expert_ids[:, :, None] == expert_of[None, None, :]
    named_any = jnp.any(named, axis=1).astype(BF16)
    token = jnp.arange(tok, dtype=jnp.int32)
    earlier = (token[None, :] < token[:, None]).astype(BF16)
    rank_all = jnp.dot(earlier, named_any, preferred_element_type=F32)
    rank = jnp.sum(jnp.where(named, rank_all[:, None, :], 0.0), axis=2).astype(jnp.int32)
    slot = expert_ids * cap + rank
    slots = experts * cap
    place = jnp.arange(slots, dtype=jnp.int32)
    spot = slot[:, :, None] == place[None, None, :]
    send_pick = jnp.any(spot, axis=1).astype(BF16)
    back_pick = jnp.sum(jnp.where(spot, route_weights[:, :, None], 0.0), axis=1).astype(BF16)

    attended = attention(queries, kvb, heads, hd)
    projected = jnp.dot(
        lax.all_gather(attended, "tp", axis=1, tiled=True), out_proj, preferred_element_type=F32
    )
    mixed = (stream.astype(F32) + projected).astype(BF16)
    mixed = lax.optimization_barrier(mixed)
    mixed_f = mixed.astype(F32)
    square_sum = lax.psum(jnp.sum(mixed_f * mixed_f, axis=1), "tp")
    inv_rms = lax.rsqrt(square_sum / width + EPS)
    normed = (mixed_f * inv_rms[:, None] * norm_gain[None, :]).astype(BF16)

    send = lax.dot_general(
        send_pick, normed, (((0,), (0,)), ((), ())), preferred_element_type=F32
    ).astype(BF16)
    send = send.reshape(n_sp, experts_local * cap, normed.shape[1])
    arrived = lax.all_to_all(send, "sp", split_axis=0, concat_axis=0, tiled=True)
    arrived = arrived.reshape(n_sp, experts_local, cap, -1)
    gates, ups = [], []
    for e in range(experts_local):
        rows = arrived[:, e].reshape(n_sp * cap, -1)
        gates.append(jnp.dot(rows, gate_proj[e], preferred_element_type=F32).astype(BF16))
        ups.append(jnp.dot(rows, up_proj[e], preferred_element_type=F32).astype(BF16))
    gates.append(jnp.dot(normed, shared_gate, preferred_element_type=F32).astype(BF16))
    ups.append(jnp.dot(normed, shared_up, preferred_element_type=F32).astype(BF16))
    gate_all = jnp.concatenate(gates, axis=0)
    up_all = jnp.concatenate(ups, axis=0)
    gate_up = jnp.concatenate([gate_all, up_all], axis=1)
    rows_all = gate_up.shape[0]
    parts = lax.all_to_all(
        gate_up.reshape(n_tp, rows_all // n_tp, 2 * hidden_width), "tp", 0, 0, tiled=True
    )
    total = jnp.sum(parts.astype(F32), axis=0)
    hidden = (jax.nn.silu(total[:, :hidden_width]) * total[:, hidden_width:]).astype(BF16)
    hidden = lax.all_gather(hidden, "tp", axis=0, tiled=True)
    outs = []
    for e in range(experts_local):
        rows = hidden[e * n_sp * cap : (e + 1) * n_sp * cap]
        out = jnp.dot(rows, down_proj[e], preferred_element_type=F32).astype(BF16)
        outs.append(out.reshape(n_sp, 1, cap, -1))
    expert_out = jnp.concatenate(outs, axis=1).reshape(n_sp, experts_local * cap, -1)
    returned = lax.all_to_all(expert_out, "sp", split_axis=0, concat_axis=0, tiled=True)
    returned = returned.reshape(slots, -1)
    shared_out = jnp.dot(
        hidden[experts_local * n_sp * cap :], shared_down, preferred_element_type=F32
    )
    routed = jnp.dot(back_pick, returned, preferred_element_type=F32)
    return (mixed_f + shared_out + routed).astype(BF16)


def solution(mesh):
    in_specs = (
        P("sp", "tp"),
        P("sp", "tp"),
        P("sp", "tp"),
        P("sp", "tp"),
        P("sp", "tp"),
        P(None, "tp"),
        P("tp"),
        P("sp", None),
        P("sp", None),
        P("sp", "tp", None),
        P("sp", "tp", None),
        P("sp", None, "tp"),
        P("tp", None),
        P("tp", None),
        P(None, "tp"),
    )
    return jax.shard_map(body, mesh=mesh, in_specs=in_specs, out_specs=P("sp", "tp"), check_vma=False)
```

```python
import functools

import jax
import jax.numpy as jnp
from jax import lax
from jax.experimental import pallas as pl
from jax.experimental.pallas import tpu as pltpu
from jax.sharding import PartitionSpec as P

EPS = 1e-06
F32 = jnp.float32
BF16 = jnp.bfloat16


def attention_kernel(
    heads, hd, n_sp, inner, q_ref, k_ref, v_ref, b_ref, o_ref, kbuf, vbuf, bbuf, acc, carry, send_sem, recv_sem
):
    tok = q_ref.shape[0]
    own = lax.axis_index("sp")
    outer = n_sp // inner
    z_own = own // inner
    x_own = own % inner
    above = z_own < outer - 1
    below = z_own > 0

    barrier = pltpu.get_barrier_semaphore()

    def greet(target):
        pl.semaphore_signal(
            barrier, inc=1, device_id={"sp": target}, device_id_type=pl.DeviceIdType.MESH
        )

    @pl.when(above)
    def _():
        greet(own + inner)

    @pl.when(below)
    def _():
        greet(own - inner)

    for d in range(1, inner):
        greet(z_own * inner + (x_own + d) % inner)
    pl.semaphore_wait(barrier, inner - 1 + above.astype(jnp.int32) + below.astype(jnp.int32))

    def copies(sources, block, z_block, lane, target):
        return [
            pltpu.make_async_remote_copy(
                src_ref=src,
                dst_ref=dst.at[block],
                send_sem=send_sem.at[kind, z_block, lane],
                recv_sem=recv_sem.at[kind, block],
                device_id={"sp": target},
                device_id_type=pl.DeviceIdType.MESH,
            )
            for kind, (src, dst) in enumerate(zip(sources, (kbuf, vbuf, bbuf)))
        ]

    def held(block):
        return (kbuf.at[block], vbuf.at[block], bbuf.at[block])

    def start_all(group):
        for c in group:
            c.start()

    def wait_sent(group):
        for c in group:
            c.wait_send()

    def wait_arrived(block):
        for c in copies(held(block), block, 0, 0, (own + 1) % n_sp):
            c.wait_recv()

    def own_sends(act):
        mine = (k_ref, v_ref, b_ref)

        @pl.when(above)
        def _():
            act(copies(mine, own, z_own, 0, own + inner))

        for d in range(1, inner):
            x_to = (x_own + d) % inner

            @pl.when(x_to > x_own)
            def _():
                act(copies(mine, own, z_own, d, z_own * inner + x_to))

    def relays(z_block, act):
        block = z_block * inner + x_own

        @pl.when(above)
        def _():
            act(copies(held(block), block, z_block, 0, own + inner))

        for d in range(1, inner):
            act(copies(held(block), block, z_block, d, z_own * inner + (x_own + d) % inner))

    own_sends(start_all)

    scale = hd ** (-0.5)
    row = lax.broadcasted_iota(jnp.int32, (tok, tok), 0)
    col = lax.broadcasted_iota(jnp.int32, (tok, tok), 1)
    later = (row > col).astype(F32)
    sums = jnp.concatenate([later, jnp.ones((tok, tok), F32)], axis=1).astype(BF16)
    sums = jnp.concatenate([sums, sums], axis=0)
    pick_rows = max(16, heads)
    pick = (
        lax.broadcasted_iota(jnp.int32, (pick_rows, hd), 0)
        == lax.broadcasted_iota(jnp.int32, (pick_rows, hd), 1)
    ).astype(F32).astype(BF16)
    acc[...] = jnp.zeros_like(acc)
    carry[...] = jnp.zeros_like(carry)

    def compute(keys, values, offsets, diagonal):
        bias = lax.dot_general(
            pick, offsets[...], (((1,), (1,)), ((), ())), preferred_element_type=F32
        )
        for h in range(heads):
            cols = slice(h * hd, (h + 1) * hd)
            z = lax.dot_general(
                q_ref[:, cols], keys[:, cols], (((1,), (1,)), ((), ())), preferred_element_type=F32
            )
            z = z * scale + bias[h : h + 1, :]
            low = jnp.log1p(jnp.exp(-jnp.abs(z)))
            fail = -(jnp.maximum(z, 0.0) + low)
            hit = jnp.minimum(z, 0.0) - low
            if diagonal:
                before = col < row
                fail = jnp.where(before, fail, 0.0)
            high = fail.astype(BF16)
            rest = (fail - high.astype(F32)).astype(BF16)
            both = jnp.dot(
                jnp.concatenate([high, rest], axis=1), sums, preferred_element_type=F32
            )
            before_sum = carry[h]
            w = jnp.exp(hit + both[:, :tok] + before_sum)
            if diagonal:
                w = jnp.where(before, w, 0.0)
            carry[h] = before_sum + both[:, tok:]
            acc[:, cols] += jnp.dot(w.astype(BF16), values[:, cols], preferred_element_type=F32)

    compute(k_ref, v_ref, b_ref, True)

    def group(i, _):
        z_block = z_own - i

        @pl.when(z_block > 0)
        def _():
            wait_arrived((z_block - 1) * inner + x_own)
            relays(z_block - 1, start_all)

        def member(m, _):
            x_block = inner - 1 - m
            block = z_block * inner + x_block

            @pl.when(block < own)
            def _():
                @pl.when(x_block != x_own)
                def _():
                    wait_arrived(block)

                compute(*held(block), False)

            return 0

        lax.fori_loop(0, inner, member, 0)
        return 0

    lax.fori_loop(0, z_own + 1, group, 0)
    o_ref[...] = acc[...].astype(BF16)

    own_sends(wait_sent)

    def drain(z_block, _):
        relays(z_block, wait_sent)
        return 0

    lax.fori_loop(0, z_own, drain, 0)


def attention(queries, keys, values, bias, heads, hd, n_sp):
    tok = queries.shape[0]
    inner = max(d for d in range(1, n_sp + 1) if n_sp % d == 0 and d * d <= n_sp)
    vmem = pl.BlockSpec(memory_space=pltpu.VMEM)
    return pl.pallas_call(
        functools.partial(attention_kernel, heads, hd, n_sp, inner),
        out_shape=jax.ShapeDtypeStruct((tok, heads * hd), BF16),
        in_specs=[vmem] * 4,
        out_specs=vmem,
        scratch_shapes=[
            pltpu.VMEM((n_sp, tok, heads * hd), BF16),
            pltpu.VMEM((n_sp, tok, heads * hd), BF16),
            pltpu.VMEM((n_sp, tok, hd), BF16),
            pltpu.VMEM((tok, heads * hd), F32),
            pltpu.VMEM((heads, tok, tok), F32),
            pltpu.SemaphoreType.DMA((3, n_sp // inner, inner)),
            pltpu.SemaphoreType.DMA((3, n_sp)),
        ],
        compiler_params=pltpu.CompilerParams(
            vmem_limit_bytes=40 * 2**20, collective_id=0, has_side_effects=True
        ),
        cost_estimate=pl.CostEstimate(flops=2 * 10**9, bytes_accessed=2**22, transcendentals=10**6),
    )(queries, keys, values, bias)


def body(
    queries,
    key_rows,
    value_rows,
    break_bias,
    stream,
    out_proj,
    norm_gain,
    expert_ids,
    route_weights,
    gate_proj,
    up_proj,
    down_proj,
    shared_gate,
    shared_up,
    shared_down,
):
    tok = queries.shape[0]
    heads = break_bias.shape[1]
    hd = queries.shape[1] // heads
    n_sp = lax.axis_size("sp")
    n_tp = lax.axis_size("tp")
    width = stream.shape[1] * n_tp
    hidden_width = gate_proj.shape[2]

    bias_wide = jnp.pad(break_bias, ((0, 0), (0, hd - heads)))

    experts_local = gate_proj.shape[0]
    experts = experts_local * n_sp
    top_k = expert_ids.shape[1]
    cap = 2 * top_k * tok // experts
    expert_of = jnp.arange(experts, dtype=jnp.int32)
    named = expert_ids[:, :, None] == expert_of[None, None, :]
    named_any = jnp.any(named, axis=1).astype(BF16)
    token = jnp.arange(tok, dtype=jnp.int32)
    earlier = (token[None, :] < token[:, None]).astype(BF16)
    rank_all = jnp.dot(earlier, named_any, preferred_element_type=F32)
    rank = jnp.sum(jnp.where(named, rank_all[:, None, :], 0.0), axis=2).astype(jnp.int32)
    slot = expert_ids * cap + rank
    slots = experts * cap
    place = jnp.arange(slots, dtype=jnp.int32)
    spot = slot[:, :, None] == place[None, None, :]
    send_pick = jnp.any(spot, axis=1).astype(BF16)
    back_pick = jnp.sum(jnp.where(spot, route_weights[:, :, None], 0.0), axis=1).astype(BF16)

    attended = attention(queries, key_rows, value_rows, bias_wide, heads, hd, n_sp)
    projected = jnp.dot(
        lax.all_gather(attended, "tp", axis=1, tiled=True), out_proj, preferred_element_type=F32
    )
    mixed = (stream.astype(F32) + projected).astype(BF16)
    mixed = lax.optimization_barrier(mixed)
    mixed_f = mixed.astype(F32)
    square_sum = lax.psum(jnp.sum(mixed_f * mixed_f, axis=1), "tp")
    inv_rms = lax.rsqrt(square_sum / width + EPS)
    normed = (mixed_f * inv_rms[:, None] * norm_gain[None, :]).astype(BF16)

    send = lax.dot_general(
        send_pick, normed, (((0,), (0,)), ((), ())), preferred_element_type=F32
    ).astype(BF16)
    send = send.reshape(n_sp, experts_local * cap, normed.shape[1])
    arrived = lax.all_to_all(send, "sp", split_axis=0, concat_axis=0, tiled=True)
    arrived = arrived.reshape(n_sp, experts_local, cap, -1)
    gates, ups = [], []
    for e in range(experts_local):
        rows = arrived[:, e].reshape(n_sp * cap, -1)
        gates.append(jnp.dot(rows, gate_proj[e], preferred_element_type=F32).astype(BF16))
        ups.append(jnp.dot(rows, up_proj[e], preferred_element_type=F32).astype(BF16))
    gates.append(jnp.dot(normed, shared_gate, preferred_element_type=F32).astype(BF16))
    ups.append(jnp.dot(normed, shared_up, preferred_element_type=F32).astype(BF16))
    gate_all = jnp.concatenate(gates, axis=0)
    up_all = jnp.concatenate(ups, axis=0)
    gate_up = jnp.concatenate([gate_all, up_all], axis=1)
    rows_all = gate_up.shape[0]
    parts = lax.all_to_all(
        gate_up.reshape(n_tp, rows_all // n_tp, 2 * hidden_width), "tp", 0, 0, tiled=True
    )
    total = jnp.sum(parts.astype(F32), axis=0)
    hidden = (jax.nn.silu(total[:, :hidden_width]) * total[:, hidden_width:]).astype(BF16)
    hidden = lax.all_gather(hidden, "tp", axis=0, tiled=True)
    outs = []
    for e in range(experts_local):
        rows = hidden[e * n_sp * cap : (e + 1) * n_sp * cap]
        out = jnp.dot(rows, down_proj[e], preferred_element_type=F32).astype(BF16)
        outs.append(out.reshape(n_sp, 1, cap, -1))
    expert_out = jnp.concatenate(outs, axis=1).reshape(n_sp, experts_local * cap, -1)
    returned = lax.all_to_all(expert_out, "sp", split_axis=0, concat_axis=0, tiled=True)
    returned = returned.reshape(slots, -1)
    shared_out = jnp.dot(
        hidden[experts_local * n_sp * cap :], shared_down, preferred_element_type=F32
    )
    routed = jnp.dot(back_pick, returned, preferred_element_type=F32)
    return (mixed_f + shared_out + routed).astype(BF16)


def solution(mesh):
    in_specs = (
        P("sp", "tp"),
        P("sp", "tp"),
        P("sp", "tp"),
        P("sp", "tp"),
        P("sp", "tp"),
        P(None, "tp"),
        P("tp"),
        P("sp", None),
        P("sp", None),
        P("sp", "tp", None),
        P("sp", "tp", None),
        P("sp", None, "tp"),
        P("tp", None),
        P("tp", None),
        P(None, "tp"),
    )
    return jax.shard_map(body, mesh=mesh, in_specs=in_specs, out_specs=P("sp", "tp"), check_vma=False)
```

```python
import functools

import jax
import jax.numpy as jnp
from jax import lax
from jax.experimental import pallas as pl
from jax.experimental.pallas import tpu as pltpu
from jax.sharding import PartitionSpec as P

EPS = 1e-06
F32 = jnp.float32
BF16 = jnp.bfloat16


def attention_kernel(
    heads, hd, n_sp, inner, q_ref, k_ref, v_ref, b_ref, o_ref, kbuf, vbuf, bbuf, acc, carry, send_sem, recv_sem
):
    tok = q_ref.shape[0]
    own = lax.axis_index("sp")
    outer = n_sp // inner
    z_own = own // inner
    x_own = own % inner
    above = z_own < outer - 1
    below = z_own > 0

    barrier = pltpu.get_barrier_semaphore()

    def greet(target):
        pl.semaphore_signal(
            barrier, inc=1, device_id={"sp": target}, device_id_type=pl.DeviceIdType.MESH
        )

    @pl.when(above)
    def _():
        greet(own + inner)

    @pl.when(below)
    def _():
        greet(own - inner)

    for d in range(1, inner):
        greet(z_own * inner + (x_own + d) % inner)
    pl.semaphore_wait(barrier, inner - 1 + above.astype(jnp.int32) + below.astype(jnp.int32))

    def copies(sources, block, z_block, lane, target):
        return [
            pltpu.make_async_remote_copy(
                src_ref=src,
                dst_ref=dst.at[block],
                send_sem=send_sem.at[kind, z_block, lane],
                recv_sem=recv_sem.at[kind, block],
                device_id={"sp": target},
                device_id_type=pl.DeviceIdType.MESH,
            )
            for kind, (src, dst) in enumerate(zip(sources, (kbuf, vbuf, bbuf)))
        ]

    def held(block):
        return (kbuf.at[block], vbuf.at[block], bbuf.at[block])

    def start_all(group):
        for c in group:
            c.start()

    def wait_sent(group):
        for c in group:
            c.wait_send()

    def wait_arrived(block):
        for c in copies(held(block), block, 0, 0, (own + 1) % n_sp):
            c.wait_recv()

    def own_sends(act):
        mine = (k_ref, v_ref, b_ref)

        @pl.when(above)
        def _():
            act(copies(mine, own, z_own, 0, own + inner))

        for d in range(1, inner):
            x_to = (x_own + d) % inner

            @pl.when(x_to > x_own)
            def _():
                act(copies(mine, own, z_own, d, z_own * inner + x_to))

    def relays(z_block, act):
        block = z_block * inner + x_own

        @pl.when(above)
        def _():
            act(copies(held(block), block, z_block, 0, own + inner))

        for d in range(1, inner):
            act(copies(held(block), block, z_block, d, z_own * inner + (x_own + d) % inner))

    own_sends(start_all)

    scale = hd ** (-0.5)
    row = lax.broadcasted_iota(jnp.int32, (tok, tok), 0)
    col = lax.broadcasted_iota(jnp.int32, (tok, tok), 1)
    later = (row > col).astype(F32)
    sums = jnp.concatenate([later, jnp.ones((tok, tok), F32)], axis=1).astype(BF16)
    sums = jnp.concatenate([sums, sums], axis=0)
    pick_rows = max(16, heads)
    pick = (
        lax.broadcasted_iota(jnp.int32, (pick_rows, hd), 0)
        == lax.broadcasted_iota(jnp.int32, (pick_rows, hd), 1)
    ).astype(F32).astype(BF16)
    acc[...] = jnp.zeros_like(acc)
    carry[...] = jnp.zeros_like(carry)

    def compute(keys, values, offsets, diagonal):
        bias = lax.dot_general(
            pick, offsets[...], (((1,), (1,)), ((), ())), preferred_element_type=F32
        )
        for h in range(heads):
            cols = slice(h * hd, (h + 1) * hd)
            z = lax.dot_general(
                q_ref[:, cols], keys[:, cols], (((1,), (1,)), ((), ())), preferred_element_type=F32
            )
            z = z * scale + bias[h : h + 1, :]
            low = jnp.log1p(jnp.exp(-jnp.abs(z)))
            fail = -(jnp.maximum(z, 0.0) + low)
            hit = jnp.minimum(z, 0.0) - low
            if diagonal:
                before = col < row
                fail = jnp.where(before, fail, 0.0)
            high = fail.astype(BF16)
            rest = (fail - high.astype(F32)).astype(BF16)
            both = jnp.dot(
                jnp.concatenate([high, rest], axis=1), sums, preferred_element_type=F32
            )
            before_sum = carry[h]
            w = jnp.exp(hit + both[:, :tok] + before_sum)
            if diagonal:
                w = jnp.where(before, w, 0.0)
            carry[h] = before_sum + both[:, tok:]
            acc[:, cols] += jnp.dot(w.astype(BF16), values[:, cols], preferred_element_type=F32)

    compute(k_ref, v_ref, b_ref, True)

    def group(i, _):
        z_block = z_own - i

        @pl.when(z_block > 0)
        def _():
            wait_arrived((z_block - 1) * inner + x_own)
            relays(z_block - 1, start_all)

        def member(m, _):
            x_block = inner - 1 - m
            block = z_block * inner + x_block

            @pl.when(block < own)
            def _():
                @pl.when(x_block != x_own)
                def _():
                    wait_arrived(block)

                compute(*held(block), False)

            return 0

        lax.fori_loop(0, inner, member, 0)
        return 0

    lax.fori_loop(0, z_own + 1, group, 0)
    o_ref[...] = acc[...].astype(BF16)

    own_sends(wait_sent)

    def drain(z_block, _):
        relays(z_block, wait_sent)
        return 0

    lax.fori_loop(0, z_own, drain, 0)


def attention(queries, keys, values, bias, heads, hd, n_sp):
    tok = queries.shape[0]
    inner = max(d for d in range(1, n_sp + 1) if n_sp % d == 0 and d * d <= n_sp)
    vmem = pl.BlockSpec(memory_space=pltpu.VMEM)
    return pl.pallas_call(
        functools.partial(attention_kernel, heads, hd, n_sp, inner),
        out_shape=jax.ShapeDtypeStruct((tok, heads * hd), BF16),
        in_specs=[vmem] * 4,
        out_specs=vmem,
        scratch_shapes=[
            pltpu.VMEM((n_sp, tok, heads * hd), BF16),
            pltpu.VMEM((n_sp, tok, heads * hd), BF16),
            pltpu.VMEM((n_sp, tok, hd), BF16),
            pltpu.VMEM((tok, heads * hd), F32),
            pltpu.VMEM((heads, tok, tok), F32),
            pltpu.SemaphoreType.DMA((3, n_sp // inner, inner)),
            pltpu.SemaphoreType.DMA((3, n_sp)),
        ],
        compiler_params=pltpu.CompilerParams(
            vmem_limit_bytes=40 * 2**20, collective_id=0, has_side_effects=True
        ),
        cost_estimate=pl.CostEstimate(flops=2 * 10**9, bytes_accessed=2**22, transcendentals=10**6),
    )(queries, keys, values, bias)


def exchange_kernel(n_tp, gu_ref, o_ref, parts, mine, spread, send_parts, recv_parts, send_rows, recv_rows):
    width = gu_ref.shape[2] // 2
    me = lax.axis_index("tp")
    barrier = pltpu.get_barrier_semaphore()
    others = [(me + d) % n_tp for d in range(1, n_tp)]
    for to in others:
        pl.semaphore_signal(
            barrier, inc=1, device_id={"tp": to}, device_id_type=pl.DeviceIdType.MESH
        )
    pl.semaphore_wait(barrier, n_tp - 1)
    first, second = [], []
    for d, to in enumerate(others):
        copy = pltpu.make_async_remote_copy(
            src_ref=gu_ref.at[to],
            dst_ref=parts.at[d],
            send_sem=send_parts.at[d],
            recv_sem=recv_parts.at[d],
            device_id={"tp": to},
            device_id_type=pl.DeviceIdType.MESH,
        )
        copy.start()
        first.append(copy)
    total = gu_ref[me].astype(F32)
    for d, copy in enumerate(first):
        copy.wait_recv()
        total = total + parts[d].astype(F32)
    gate = total[:, :width]
    mine[...] = (jax.nn.silu(gate) * total[:, width:]).astype(BF16)
    for d, to in enumerate(others):
        copy = pltpu.make_async_remote_copy(
            src_ref=mine,
            dst_ref=spread.at[d],
            send_sem=send_rows.at[d],
            recv_sem=recv_rows.at[d],
            device_id={"tp": to},
            device_id_type=pl.DeviceIdType.MESH,
        )
        copy.start()
        second.append(copy)
    o_ref[me] = mine[...]
    for d, copy in enumerate(second):
        copy.wait_recv()
        o_ref[(me + n_tp - 1 - d) % n_tp] = spread[d]
    for copy in first + second:
        copy.wait_send()


def exchange(gate_up, n_tp):
    rows, width = gate_up.shape[0] // n_tp, gate_up.shape[1] // 2
    vmem = pl.BlockSpec(memory_space=pltpu.VMEM)
    dma = pltpu.SemaphoreType.DMA((n_tp - 1,))
    hidden = pl.pallas_call(
        functools.partial(exchange_kernel, n_tp),
        out_shape=jax.ShapeDtypeStruct((n_tp, rows, width), BF16),
        in_specs=[vmem],
        out_specs=vmem,
        scratch_shapes=[
            pltpu.VMEM((n_tp - 1, rows, 2 * width), BF16),
            pltpu.VMEM((rows, width), BF16),
            pltpu.VMEM((n_tp - 1, rows, width), BF16),
            dma,
            dma,
            dma,
            dma,
        ],
        compiler_params=pltpu.CompilerParams(
            vmem_limit_bytes=24 * 2**20, collective_id=1, has_side_effects=True
        ),
        cost_estimate=pl.CostEstimate(flops=10**8, bytes_accessed=2**21, transcendentals=10**5),
    )(gate_up.reshape(n_tp, rows, 2 * width))
    return hidden.reshape(n_tp * rows, width)


def body(
    queries,
    key_rows,
    value_rows,
    break_bias,
    stream,
    out_proj,
    norm_gain,
    expert_ids,
    route_weights,
    gate_proj,
    up_proj,
    down_proj,
    shared_gate,
    shared_up,
    shared_down,
):
    tok = queries.shape[0]
    heads = break_bias.shape[1]
    hd = queries.shape[1] // heads
    n_sp = lax.axis_size("sp")
    n_tp = lax.axis_size("tp")
    width = stream.shape[1] * n_tp

    bias_wide = jnp.pad(break_bias, ((0, 0), (0, hd - heads)))

    experts_local = gate_proj.shape[0]
    experts = experts_local * n_sp
    top_k = expert_ids.shape[1]
    cap = 2 * top_k * tok // experts
    expert_of = jnp.arange(experts, dtype=jnp.int32)
    named = expert_ids[:, :, None] == expert_of[None, None, :]
    named_any = jnp.any(named, axis=1).astype(BF16)
    token = jnp.arange(tok, dtype=jnp.int32)
    earlier = (token[None, :] < token[:, None]).astype(BF16)
    rank_all = jnp.dot(earlier, named_any, preferred_element_type=F32)
    rank = jnp.sum(jnp.where(named, rank_all[:, None, :], 0.0), axis=2).astype(jnp.int32)
    slot = expert_ids * cap + rank
    slots = experts * cap
    place = jnp.arange(slots, dtype=jnp.int32)
    spot = slot[:, :, None] == place[None, None, :]
    send_pick = jnp.any(spot, axis=1).astype(BF16)
    back_pick = jnp.sum(jnp.where(spot, route_weights[:, :, None], 0.0), axis=1).astype(BF16)

    attended = attention(queries, key_rows, value_rows, bias_wide, heads, hd, n_sp)
    projected = jnp.dot(
        lax.all_gather(attended, "tp", axis=1, tiled=True), out_proj, preferred_element_type=F32
    )
    mixed = (stream.astype(F32) + projected).astype(BF16)
    mixed = lax.optimization_barrier(mixed)
    mixed_f = mixed.astype(F32)
    square_sum = lax.psum(jnp.sum(mixed_f * mixed_f, axis=1), "tp")
    inv_rms = lax.rsqrt(square_sum / width + EPS)
    normed = (mixed_f * inv_rms[:, None] * norm_gain[None, :]).astype(BF16)

    send = lax.dot_general(
        send_pick, normed, (((0,), (0,)), ((), ())), preferred_element_type=F32
    ).astype(BF16)
    send = send.reshape(n_sp, experts_local * cap, normed.shape[1])
    arrived = lax.all_to_all(send, "sp", split_axis=0, concat_axis=0, tiled=True)
    arrived = arrived.reshape(n_sp, experts_local, cap, -1)
    gates, ups = [], []
    for e in range(experts_local):
        rows = arrived[:, e].reshape(n_sp * cap, -1)
        gates.append(jnp.dot(rows, gate_proj[e], preferred_element_type=F32).astype(BF16))
        ups.append(jnp.dot(rows, up_proj[e], preferred_element_type=F32).astype(BF16))
    gates.append(jnp.dot(normed, shared_gate, preferred_element_type=F32).astype(BF16))
    ups.append(jnp.dot(normed, shared_up, preferred_element_type=F32).astype(BF16))
    gate_all = jnp.concatenate(gates, axis=0)
    up_all = jnp.concatenate(ups, axis=0)
    gate_up = jnp.concatenate([gate_all, up_all], axis=1)
    hidden = exchange(gate_up, n_tp)
    outs = []
    for e in range(experts_local):
        rows = hidden[e * n_sp * cap : (e + 1) * n_sp * cap]
        out = jnp.dot(rows, down_proj[e], preferred_element_type=F32).astype(BF16)
        outs.append(out.reshape(n_sp, 1, cap, -1))
    expert_out = jnp.concatenate(outs, axis=1).reshape(n_sp, experts_local * cap, -1)
    returned = lax.all_to_all(expert_out, "sp", split_axis=0, concat_axis=0, tiled=True)
    returned = returned.reshape(slots, -1)
    shared_out = jnp.dot(
        hidden[experts_local * n_sp * cap :], shared_down, preferred_element_type=F32
    )
    routed = jnp.dot(back_pick, returned, preferred_element_type=F32)
    return (mixed_f + shared_out + routed).astype(BF16)


def solution(mesh):
    in_specs = (
        P("sp", "tp"),
        P("sp", "tp"),
        P("sp", "tp"),
        P("sp", "tp"),
        P("sp", "tp"),
        P(None, "tp"),
        P("tp"),
        P("sp", None),
        P("sp", None),
        P("sp", "tp", None),
        P("sp", "tp", None),
        P("sp", None, "tp"),
        P("tp", None),
        P("tp", None),
        P(None, "tp"),
    )
    return jax.shard_map(body, mesh=mesh, in_specs=in_specs, out_specs=P("sp", "tp"), check_vma=False)
```
